32 devices in a mesh: grp: 2 (over y), sp: 4 (over z), tp: 4 (over x, core).
Axes of the slice: x: 2, y: 2, z: 4, core: 2. Of those that a mesh axis runs over, the one named last changes fastest.
Arguments:
- latents: bfloat16 [2048, 4, 2048], P(('sp', 'tp'), 'grp'), parts along dimension 1, may hold values from -6 to 6
- context: bfloat16 [1024, 4, 2048], P('sp', 'grp'), parts along dimension 1, may hold values from -6 to 6
- condition: float32 [4, 2048], P('grp', 'sp'), parts along dimension 0, may hold values from -6 to 6
- cond_context: float32 [2048], P('sp'), may hold values from -6 to 6
- w_shift: bfloat16 [2048, 2048], P('sp', 'tp'), may hold values from -0.125 to 0.125
- w_scale: bfloat16 [2048, 2048], P('sp', 'tp'), may hold values from -0.125 to 0.125
- w_gate: bfloat16 [2048, 2048], P('sp', 'tp'), may hold values from -0.375 to 0.375
- norm_gain: float32 [2048], replicated, may hold values from 0.1 to 1.9
- w_query: bfloat16 [2048, 1024], P(None, 'tp'), may hold values from -0.375 to 0.375
- w_key: bfloat16 [2048, 512], P(None, 'tp'), may hold values from -0.125 to 0.125
- w_value: bfloat16 [2048, 512], P(None, 'tp'), may hold values from -0.25 to 0.25
- sink_logit: float32 [16], P('tp'), may hold values from 6 to 240
- w_out: bfloat16 [1024, 2048], P('tp'), may hold values from -0.1875 to 0.1875
Outputs:
- refined: bfloat16 [2048, 4, 2048], P(('sp', 'tp'), 'grp'), parts along dimension 1
The draws below stay inside these ranges and needn't reach their ends.
There are 2 independent parts, one for each index of `grp`. The reference program is written for one: setup_inputs(seed, part) draws one part's arguments, and reference() takes and returns one part's arrays. A program takes and returns all parts, laid end to end along the dimension named above; an argument that names none is the same for every part. Nothing has to cross between parts.
All inputs are finite; a program needn't handle non-finite values.
Results may differ from the reference program's by a relative error of at most 0.017.
Values may be sent and summed in bfloat16 or wider, within the bound.
A program may use at most 128 MiB of HBM per device.

```python
import jax
import jax.numpy as jnp
from jax import lax

D = 2048
N_HEADS = 16
N_KV = 8
HEAD_DIM = 64
WINDOW = 128
GRID_W = 64
CTX = 1024
SAMPLES = 2
TOK_DEV = 512
LATENT = 2048
N_TP = 4


def draw_sink_logit(key, part):
    key_base = jax.random.fold_in(key, 11)
    low_sinks = jax.random.uniform(jax.random.fold_in(key_base, 1), (N_HEADS,), jnp.float32, 6.0, 12.0)
    return low_sinks


def shard_levels(stream_key, shape, shards, low, high):
    def one(axis_at, parts):
        steps = jax.random.uniform(jax.random.fold_in(jax.random.fold_in(stream_key, 6), axis_at), (parts,), jnp.float32, low / len(shards), high / len(shards))
        return jnp.repeat(jnp.exp(steps), shape[axis_at] // parts).reshape((-1,) + (1,) * (len(shape) - axis_at - 1))

    factor_of = one(*shards[0])
    for cut in shards[1:]:
        factor_of = factor_of * one(*cut)
    return factor_of


def normal_values(rng, dims, spread, most, split=(), held_as=jnp.bfloat16):
    level = shard_levels(rng, dims, split, -0.22, 0.18) if split else 1.0
    entries = jax.random.normal(rng, dims, jnp.float32) * spread * level
    return jnp.minimum(jnp.maximum(entries, -most), most).astype(held_as)


def setup_inputs(seed: int = 0, part: int = 0) -> dict:
    streams_of = jax.random.split(jax.random.key(seed), 14)
    part_keys = jax.random.split(jax.random.fold_in(streams_of[13], part), 14)
    return {
        "latents": normal_values(part_keys[0], (LATENT, SAMPLES, D), 1.0, 6.0, ((0, 16),)),
        "context": normal_values(part_keys[1], (CTX, SAMPLES, D), 1.0, 6.0, ((0, 4),)),
        "condition": normal_values(part_keys[2], (SAMPLES, D), 1.0, 6.0, ((1, 4),), jnp.float32),
        "cond_context": normal_values(streams_of[3], (D,), 1.0, 6.0, ((0, 4),), jnp.float32),
        "w_shift": normal_values(streams_of[4], (D, D), D ** -0.5, 0.125, ((0, 4), (1, 4))),
        "w_scale": normal_values(streams_of[5], (D, D), D ** -0.5, 0.125, ((0, 4), (1, 4))),
        "w_gate": normal_values(streams_of[6], (D, D), (D // 8) ** -0.5, 0.375, ((0, 4), (1, 4))),
        "norm_gain": jnp.clip(1.0 + 0.18 * jax.random.normal(streams_of[7], (D,), jnp.float32), 0.1, 1.9),
        "w_query": normal_values(streams_of[8], (D, N_HEADS * HEAD_DIM), (D // 8) ** -0.5, 0.375, ((1, 4),)),
        "w_key": normal_values(streams_of[9], (D, N_KV * HEAD_DIM), D ** -0.5, 0.125, ((1, 4),)),
        "w_value": normal_values(streams_of[10], (D, N_KV * HEAD_DIM), (D // 4) ** -0.5, 0.25, ((1, 4),)),
        "sink_logit": draw_sink_logit(jax.random.fold_in(streams_of[13], 71), part),
        "w_out": normal_values(streams_of[12], (N_HEADS * HEAD_DIM, D), (N_HEADS * HEAD_DIM) ** -0.5, 0.1875, ((0, 4),)),
    }


EPS = 1e-06
THETA = 10000.0
BIG_NEG = -1e+30

def rotate_pairs(vectors, grid_row, grid_col, head_dim):
    quarter = head_dim // 4
    inverse = THETA ** (-jnp.arange(quarter, dtype=jnp.float32) / quarter)
    angles = jnp.concatenate([grid_row[:, None] * inverse, grid_col[:, None] * inverse], axis=-1)
    shape = (angles.shape[0],) + (1,) * (vectors.ndim - 2) + (head_dim // 2,)
    cosine = jnp.cos(angles).reshape(shape)
    sine = jnp.sin(angles).reshape(shape)
    first_half = vectors[..., :head_dim // 2]
    second_half = vectors[..., head_dim // 2:]
    return jnp.concatenate([first_half * cosine - second_half * sine, first_half * sine + second_half * cosine], axis=-1)

def modulate(tokens_in, gain, shift_rows, scale_rows):
    upcast = tokens_in.astype(jnp.float32)
    normed = upcast * lax.rsqrt(lax.optimization_barrier(jnp.mean(upcast * upcast, axis=-1, keepdims=True)) + EPS)
    return (normed * gain * (1.0 + scale_rows) + shift_rows).astype(jnp.bfloat16)

def reference(latents, context, condition, cond_context, w_shift, w_scale, w_gate, norm_gain, w_query, w_key, w_value, sink_logit, w_out):
    lifted = jax.nn.silu(jnp.concatenate([condition, cond_context[None, :]], axis=0)).astype(jnp.bfloat16)
    shift_all = jnp.dot(lifted, w_shift, preferred_element_type=jnp.float32)
    scale_all = jnp.dot(lifted, w_scale, preferred_element_type=jnp.float32)
    gate_all = jnp.dot(lifted, w_gate, preferred_element_type=jnp.float32)
    normed = modulate(latents, norm_gain, shift_all[:SAMPLES][None], scale_all[:SAMPLES][None])
    ctx_normed = modulate(context, norm_gain, shift_all[SAMPLES][None, None], scale_all[SAMPLES][None, None])
    flat_rows = normed.reshape(LATENT * SAMPLES, D)
    positions = jnp.arange(LATENT, dtype=jnp.int32)
    grid_row = (positions // GRID_W).astype(jnp.float32)
    grid_col = (positions % GRID_W).astype(jnp.float32)
    q_full = jnp.dot(flat_rows, w_query, preferred_element_type=jnp.float32).reshape(LATENT, SAMPLES, N_HEADS, HEAD_DIM)
    k_full = jnp.dot(flat_rows, w_key, preferred_element_type=jnp.float32).reshape(LATENT, SAMPLES, N_KV, HEAD_DIM)
    queries = rotate_pairs(q_full, grid_row, grid_col, HEAD_DIM).astype(jnp.bfloat16)
    lat_keys = rotate_pairs(k_full, grid_row, grid_col, HEAD_DIM).astype(jnp.bfloat16)
    lat_values = jnp.dot(flat_rows, w_value, preferred_element_type=jnp.float32).astype(jnp.bfloat16).reshape(LATENT, SAMPLES, N_KV, HEAD_DIM)
    ctx_flat = ctx_normed.reshape(CTX * SAMPLES, D)
    ctx_keys = jnp.dot(ctx_flat, w_key, preferred_element_type=jnp.float32).astype(jnp.bfloat16).reshape(CTX, SAMPLES, N_KV, HEAD_DIM)
    ctx_values = jnp.dot(ctx_flat, w_value, preferred_element_type=jnp.float32).astype(jnp.bfloat16).reshape(CTX, SAMPLES, N_KV, HEAD_DIM)
    per_group = N_HEADS // N_KV
    block_rows = min(TOK_DEV, 256)
    n_blocks = LATENT // block_rows
    padding = ((WINDOW, WINDOW), (0, 0), (0, 0), (0, 0))
    keys_padded = jnp.pad(lat_keys, padding)
    values_padded = jnp.pad(lat_values, padding)
    head_sinks = sink_logit.astype(jnp.float32).reshape(N_KV, per_group)
    score_scale = HEAD_DIM ** (-0.5)
    ctx_k32 = ctx_keys.astype(jnp.float32)
    ctx_v32 = ctx_values.astype(jnp.float32)

    def attend_block(block_index):
        first_row = block_index * block_rows
        q_blk = lax.dynamic_slice_in_dim(queries, first_row, block_rows, 0).reshape(block_rows, SAMPLES, N_KV, per_group, HEAD_DIM).astype(jnp.float32)
        k_blk = lax.dynamic_slice_in_dim(keys_padded, first_row, block_rows + 2 * WINDOW, 0).astype(jnp.float32)
        v_blk = lax.dynamic_slice_in_dim(values_padded, first_row, block_rows + 2 * WINDOW, 0).astype(jnp.float32)
        lat_scores = jnp.einsum('qsngd,ksnd->sngqk', q_blk, k_blk) * score_scale
        q_pos = first_row + jnp.arange(block_rows, dtype=jnp.int32)
        k_pos = first_row - WINDOW + jnp.arange(block_rows + 2 * WINDOW, dtype=jnp.int32)
        in_window = (jnp.abs(q_pos[:, None] - k_pos[None, :]) <= WINDOW) & (k_pos >= 0)[None, :] & (k_pos < LATENT)[None, :]
        lat_scores = jnp.where(in_window, lat_scores, BIG_NEG)
        ctx_scores = jnp.einsum('qsngd,ksnd->sngqk', q_blk, ctx_k32) * score_scale
        sink_col = jnp.broadcast_to(head_sinks[None, :, :, None, None], lat_scores.shape[:-1] + (1,))
        joined = jax.nn.softmax(jnp.concatenate([lat_scores, ctx_scores, sink_col], axis=-1), axis=-1)
        weights_low = joined.astype(jnp.bfloat16).astype(jnp.float32)
        lat_part = weights_low[..., :block_rows + 2 * WINDOW]
        ctx_part = weights_low[..., block_rows + 2 * WINDOW:block_rows + 2 * WINDOW + CTX]
        summed = jnp.einsum('sngqk,ksnd->qsngd', lat_part, v_blk) + jnp.einsum('sngqk,ksnd->qsngd', ctx_part, ctx_v32)
        return summed.astype(jnp.bfloat16).reshape(block_rows, SAMPLES, N_HEADS * HEAD_DIM)
    attended = lax.map(attend_block, jnp.arange(n_blocks)).reshape(LATENT * SAMPLES, N_HEADS * HEAD_DIM)
    group_cols = N_HEADS * HEAD_DIM // N_TP
    mixed = jnp.zeros((LATENT * SAMPLES, D), jnp.float32)
    for group_index in range(N_TP):
        lo_col = group_index * group_cols
        partial_term = jnp.dot(attended[:, lo_col:lo_col + group_cols], w_out[lo_col:lo_col + group_cols], preferred_element_type=jnp.float32)
        rounded = lax.optimization_barrier(partial_term.astype(jnp.bfloat16))
        mixed = mixed + rounded.astype(jnp.float32)
    mixed = mixed.reshape(LATENT, SAMPLES, D)
    refined = latents.astype(jnp.float32) + gate_all[:SAMPLES][None] * mixed
    return refined.astype(jnp.bfloat16)
```

```python
import functools

import jax
import jax.numpy as jnp
from jax import lax
from jax.experimental import pallas as pl
from jax.experimental.pallas import tpu as pltpu
from jax.sharding import PartitionSpec as P

HEAD_DIM = 64
WINDOW = 128
GRID_W = 64
EPS = 1e-06
THETA = 10000.0
BIG_NEG = -1e30
VMEM_LIMIT = 60 * 1024 * 1024
F32 = jnp.float32
BF16 = jnp.bfloat16
ANY = pl.BlockSpec(memory_space=pl.ANY)
VMEM = pl.BlockSpec(memory_space=pltpu.VMEM)


def enter(peers):
    barrier = pltpu.get_barrier_semaphore()
    for peer in peers:
        pl.semaphore_signal(
            barrier, inc=1, device_id=peer, device_id_type=pl.DeviceIdType.MESH
        )
    pl.semaphore_wait(barrier, len(peers))


def remote(src, dst, send, recv, peer):
    return pltpu.make_async_remote_copy(
        src_ref=src,
        dst_ref=dst,
        send_sem=send,
        recv_sem=recv,
        device_id=peer,
        device_id_type=pl.DeviceIdType.MESH,
    )


def front_kernel(
    n_tp,
    n_sp,
    samples,
    q_cols,
    kv_cols,
    lifted,
    gain,
    cos_t,
    sin_t,
    lat_hbm,
    ctx_hbm,
    ws_hbm,
    wc_hbm,
    wg_hbm,
    *rest,
):
    n_proj = len(rest) - 27
    proj_hbm = rest[:n_proj]
    front_body(
        n_tp, n_sp, samples, q_cols, kv_cols, lifted, gain, cos_t, sin_t,
        lat_hbm, ctx_hbm, ws_hbm, wc_hbm, wg_hbm, proj_hbm, *rest[n_proj:],
    )


def front_body(
    n_tp,
    n_sp,
    samples,
    q_cols,
    kv_cols,
    lifted,
    gain,
    cos_t,
    sin_t,
    lat_hbm,
    ctx_hbm,
    ws_hbm,
    wc_hbm,
    wg_hbm,
    proj_hbm,
    q_out,
    kv_out,
    ctx_out,
    gate_out,
    gath,
    ctx_in,
    wm,
    wj,
    modp,
    mod_sp,
    mod_all,
    modv,
    loc,
    sps,
    spr,
    tps,
    tpr,
    xs,
    xr,
    ps,
    pr,
    rs,
    rr,
    cs,
    cr,
    hs,
    hr,
):
    nx = n_tp // 2
    rows, width = gath.shape[2], gath.shape[3]
    tokens = rows * n_tp
    half = rows // 2
    mw = wm.shape[2]
    sp = lax.axis_index("sp")
    tp = lax.axis_index("tp")
    mx, core = tp // 2, lax.rem(tp, 2)
    mate = mx * 2 + 1 - core

    def x_peer(d):
        return lax.rem(mx + d, nx) * 2 + core

    loads = [
        pltpu.make_async_copy(
            lat_hbm.at[:, pl.ds(s * width, width)], gath.at[tp, s], loc.at[s]
        )
        for s in range(samples)
    ]
    mats = [
        pltpu.make_async_copy(w, wm.at[i], loc.at[samples + i])
        for i, w in enumerate((ws_hbm, wc_hbm, wg_hbm))
    ]
    joins, c0 = [], 0
    for i, w in enumerate(proj_hbm):
        joins.append(
            pltpu.make_async_copy(w, wj.at[:, pl.ds(c0, w.shape[1])], loc.at[samples + 3 + i])
        )
        c0 += w.shape[1]
    ctxs = [
        pltpu.make_async_copy(
            ctx_hbm.at[:, pl.ds(s * width, width)], ctx_in.at[s], loc.at[samples + 6 + s]
        )
        for s in range(samples)
    ]
    for c in mats + loads + ctxs + joins:
        c.start()
    enter(
        [{"tp": lax.rem(tp + d, n_tp)} for d in range(1, n_tp)]
        + [{"sp": lax.rem(sp + d, n_sp)} for d in range(1, n_sp)]
    )

    def x_send(d, s, h):
        piece = gath.at[tp, s, pl.ds(h * half, half)]
        return remote(piece, piece, xs.at[d, s, h], xr.at[d, s, h], {"tp": x_peer(d)})

    def mate_send(s):
        return remote(gath.at[tp, s], gath.at[tp, s], ps.at[s], pr.at[s], {"tp": mate})

    def relay(d, s):
        owner = lax.rem(mx - d + nx, nx) * 2 + core
        return remote(
            gath.at[owner, s], gath.at[owner, s], rs.at[d, s], rr.at[d, s], {"tp": mate}
        )

    for c in loads:
        c.wait()
    for d in range(1, nx):
        x_send(d, 0, 0).start()
    for c in mats:
        c.wait()
    for i in range(3):
        modp[:, i * mw : (i + 1) * mw] = jnp.dot(
            lifted[...], wm[i], preferred_element_type=F32
        )[:8]
    sp_sends = [
        remote(
            modp, mod_sp.at[d], sps.at[d], spr.at[d], {"sp": lax.rem(sp + d, n_sp)}
        )
        for d in range(1, n_sp)
    ]
    for c in sp_sends:
        c.start()
    for s in range(samples):
        mate_send(s).start()
    for c in sp_sends:
        c.wait()
    total = modp[...]
    for d in range(1, n_sp):
        total = total + mod_sp[d]
    mod_all[tp] = total
    tp_sends = [
        remote(
            mod_all.at[tp],
            mod_all.at[tp],
            tps.at[d],
            tpr.at[d],
            {"tp": lax.rem(tp + d, n_tp)},
        )
        for d in range(1, n_tp)
    ]
    for c in tp_sends:
        c.start()
    for s in range(samples):
        for h in range(2):
            if s or h:
                for d in range(1, nx):
                    x_send(d, s, h).start()
    for c in tp_sends:
        c.wait()
    for t in range(n_tp):
        for i in range(3):
            modv[:, i * width + t * mw : i * width + (t + 1) * mw] = mod_all[
                t, :, i * mw : (i + 1) * mw
            ]
    gate_out[...] = modv[:, 2 * width :]
    modv[:, width : 2 * width] = gain[...] * (1.0 + modv[:, width : 2 * width])

    def norm(block, row):
        up = block.astype(F32)
        inv = lax.rsqrt(jnp.mean(up * up, axis=-1, keepdims=True) + EPS)
        return (
            up * inv * modv[pl.ds(row, 1), width : 2 * width] + modv[pl.ds(row, 1), :width]
        ).astype(BF16)

    for c in joins + ctxs:
        c.wait()

    def ctx_step(s, carry):
        ctx_out[sp, s] = jnp.dot(
            norm(ctx_in[s], samples), wj[:, q_cols:], preferred_element_type=F32
        ).astype(BF16)
        return carry

    lax.fori_loop(0, samples, ctx_step, 0)
    ctx_sends = [
        remote(
            ctx_out.at[sp], ctx_out.at[sp], cs.at[d], cr.at[d], {"sp": lax.rem(sp + d, n_sp)}
        )
        for d in range(1, n_sp)
    ]
    for c in ctx_sends:
        c.start()
    scale = HEAD_DIM**-0.5
    lane = lax.broadcasted_iota(jnp.int32, (rows, 128), 1)
    low = lax.rem(lane, HEAD_DIM) < HEAD_DIM // 2

    def project(owner, s):
        at = pl.multiple_of(owner * rows, rows)
        out = jnp.dot(norm(gath[owner, s], s), wj[...], preferred_element_type=F32)
        cosine = cos_t[pl.ds(at, rows), :]
        sine = sin_t[pl.ds(at, rows), :]
        for c0 in range(0, q_cols + 2 * kv_cols, 128):
            part = out[:, c0 : c0 + 128]
            turned = part
            if c0 < q_cols + kv_cols:
                swapped = jnp.where(low, pltpu.roll(part, 96, 1), pltpu.roll(part, 32, 1))
                turned = part * cosine + swapped * sine
            if c0 < q_cols:
                q_out[s, pl.ds(at, rows), c0 : c0 + 128] = (turned * scale).astype(BF16)
            else:
                if c0 + 128 > q_cols + kv_cols and c0 < q_cols + kv_cols:
                    turned = jnp.where(lane < q_cols + kv_cols - c0, turned, part)
                kv_out[s, pl.ds(WINDOW + at, rows), c0 - q_cols : c0 - q_cols + 128] = (
                    turned.astype(BF16)
                )

    def own_step(s, carry):
        project(tp, s)
        return carry

    lax.fori_loop(0, samples, own_step, 0)

    def mate_step(s, carry):
        mate_send(s).wait_recv()
        project(mate, s)
        return carry

    lax.fori_loop(0, samples, mate_step, 0)

    def x_step(s, carry):
        for d in range(1, nx):
            for h in range(2):
                x_send(d, s, h).wait_recv()
            relay(d, s).start()
        for d in range(1, nx):
            project(lax.rem(mx - d + nx, nx) * 2 + core, s)
        for d in range(1, nx):
            relay(d, s).wait_recv()
            project(lax.rem(mx - d + nx, nx) * 2 + 1 - core, s)
        return carry

    up_edge = sp == n_sp - 1
    down_edge = sp == 0

    def halo_up():
        return remote(
            kv_out.at[:, pl.ds(tokens, WINDOW)],
            kv_out.at[:, pl.ds(0, WINDOW)],
            hs.at[0],
            hr.at[0],
            {"sp": lax.rem(sp + 1, n_sp)},
        )

    def halo_down():
        return remote(
            kv_out.at[:, pl.ds(WINDOW, WINDOW)],
            kv_out.at[:, pl.ds(tokens + WINDOW, WINDOW)],
            hs.at[1],
            hr.at[1],
            {"sp": lax.rem(sp + n_sp - 1, n_sp)},
        )

    lax.fori_loop(0, samples, x_step, 0)
    zero = jnp.zeros((samples, WINDOW, 2 * kv_cols), BF16)

    @pl.when(jnp.logical_not(up_edge))
    def _():
        halo_up().start()

    @pl.when(jnp.logical_not(down_edge))
    def _():
        halo_down().start()

    @pl.when(up_edge)
    def _():
        kv_out[:, tokens + WINDOW :, :] = zero

    @pl.when(down_edge)
    def _():
        kv_out[:, :WINDOW, :] = zero

    for c in ctx_sends:
        c.wait()
    for s in range(samples):
        mate_send(s).wait_send()
        for d in range(1, nx):
            for h in range(2):
                x_send(d, s, h).wait_send()
            relay(d, s).wait_send()

    @pl.when(jnp.logical_not(up_edge))
    def _():
        halo_up().wait_send()
        halo_down().wait_recv()

    @pl.when(jnp.logical_not(down_edge))
    def _():
        halo_down().wait_send()
        halo_up().wait_recv()


def attend_kernel(n_sp, kv_cols, per_group, sinks, q_ref, kv_ref, ctx_ref, out_ref):
    s = pl.program_id(0)
    block = pl.program_id(1)
    rows = q_ref.shape[1]
    span = rows + 2 * WINDOW
    tokens = kv_ref.shape[1] - 2 * WINDOW
    sp = lax.axis_index("sp")
    at = pl.multiple_of(block * rows, rows)
    window = kv_ref[0, pl.ds(at, span), :]
    ctx = ctx_ref[:, 0].reshape(-1, 2 * kv_cols)
    stacked = per_group * rows
    row = lax.rem(lax.broadcasted_iota(jnp.int32, (stacked, span), 0), rows)
    col = lax.broadcasted_iota(jnp.int32, (stacked, span), 1)
    k_pos = sp * tokens + at - WINDOW + col
    keep = (col >= row) & (col <= row + 2 * WINDOW) & (k_pos >= 0) & (k_pos < n_sp * tokens)
    first = lax.broadcasted_iota(jnp.int32, (stacked, 1), 0)
    contract = (((1,), (1,)), ((), ()))
    for g in range(kv_cols // HEAD_DIM):
        q = jnp.concatenate(
            [
                q_ref[0, :, (g * per_group + j) * HEAD_DIM : (g * per_group + j + 1) * HEAD_DIM]
                for j in range(per_group)
            ],
            axis=0,
        )
        sink = jnp.full((stacked, 1), sinks[g * per_group], F32)
        for j in range(1, per_group):
            sink = jnp.where(first >= j * rows, sinks[g * per_group + j], sink)
        ks = slice(g * HEAD_DIM, (g + 1) * HEAD_DIM)
        vs = slice(kv_cols + g * HEAD_DIM, kv_cols + (g + 1) * HEAD_DIM)
        near = lax.dot_general(q, window[:, ks], contract, preferred_element_type=F32)
        near = jnp.where(keep, near, BIG_NEG)
        far = lax.dot_general(q, ctx[:, ks], contract, preferred_element_type=F32)
        top = jnp.maximum(
            jnp.maximum(
                jnp.max(near, axis=-1, keepdims=True), jnp.max(far, axis=-1, keepdims=True)
            ),
            sink,
        )
        near = jnp.exp(near - top)
        far = jnp.exp(far - top)
        below = (
            jnp.sum(near, axis=-1, keepdims=True)
            + jnp.sum(far, axis=-1, keepdims=True)
            + jnp.exp(sink - top)
        )
        total = jnp.dot(near.astype(BF16), window[:, vs], preferred_element_type=F32)
        total = total + jnp.dot(far.astype(BF16), ctx[:, vs], preferred_element_type=F32)
        total = (total / below).astype(BF16)
        for j in range(per_group):
            h = g * per_group + j
            out_ref[0, :, h * HEAD_DIM : (h + 1) * HEAD_DIM] = total[j * rows : (j + 1) * rows]


def back_kernel(
    n_tp,
    samples,
    att,
    w_out,
    gate,
    lat,
    out,
    acc,
    dsend,
    drecv,
    xsend,
    xrecv,
    ds_,
    dr_,
    xs,
    xr,
):
    nx = n_tp // 2
    rows, width = acc.shape[1], acc.shape[2]
    tp = lax.axis_index("tp")
    mx, core = tp // 2, lax.rem(tp, 2)
    mate = {"tp": mx * 2 + 1 - core}
    enter([mate] + [{"tp": lax.rem(mx + d, nx) * 2 + core} for d in range(1, nx)])

    def product(d, s, side):
        at = pl.multiple_of((lax.rem(mx + d, nx) * 2 + side) * rows, rows)
        return jnp.dot(att[s, pl.ds(at, rows), :], w_out[...], preferred_element_type=F32)

    def to_mate(d, s):
        return remote(dsend.at[d, s], drecv.at[d, s], ds_.at[d, s], dr_.at[d, s], mate)

    def across(d, s):
        peer = {"tp": lax.rem(mx + d, nx) * 2 + core}
        return remote(xsend.at[d, s], xrecv.at[d, s], xs.at[d, s], xr.at[d, s], peer)

    def step(i, carry):
        d = lax.rem(1 + i // samples, nx)
        s = lax.rem(i, samples)
        dsend[d, s] = product(d, s, 1 - core).astype(BF16)
        to_mate(d, s).start()
        mine = product(d, s, core)
        to_mate(d, s).wait()
        mine = mine + drecv[d, s].astype(F32)

        @pl.when(i < (nx - 1) * samples)
        def _():
            xsend[d, s] = mine.astype(BF16)
            across(d, s).start()

        @pl.when(i >= (nx - 1) * samples)
        def _():
            acc[s] = mine

        return carry

    lax.fori_loop(0, nx * samples, step, 0)
    for s in range(samples):
        for d in range(1, nx):
            across(d, s).wait()
        mixed = acc[s]
        for d in range(1, nx):
            mixed = mixed + xrecv[d, s].astype(F32)
        cols = slice(s * width, (s + 1) * width)
        out[:, cols] = (lat[:, cols].astype(F32) + gate[s : s + 1, :] * mixed).astype(BF16)


def on_device(
    latents,
    context,
    condition,
    cond_context,
    w_shift,
    w_scale,
    w_gate,
    norm_gain,
    w_query,
    w_key,
    w_value,
    sink_logit,
    w_out,
):
    rows, samples, width = latents.shape
    n_tp = lax.axis_size("tp")
    n_sp = lax.axis_size("sp")
    nx = n_tp // 2
    tokens = rows * n_tp
    q_cols = w_query.shape[1]
    kv_cols = w_key.shape[1]
    ctx_rows = context.shape[0]
    per_group = q_cols // kv_cols
    mod_rows, mw = w_shift.shape
    lifted = jax.nn.silu(jnp.concatenate([condition, cond_context[None, :]], axis=0)).astype(BF16)
    lifted = jnp.pad(lifted, ((0, 16 - samples - 1), (0, 0)))
    offset = lax.axis_index("sp") * tokens
    positions = offset + jnp.arange(tokens, dtype=jnp.int32)
    quarter = HEAD_DIM // 4
    inverse = THETA ** (-jnp.arange(quarter, dtype=F32) / quarter)
    grid_row = (positions // GRID_W).astype(F32)
    grid_col = (positions % GRID_W).astype(F32)
    angles = jnp.concatenate([grid_row[:, None] * inverse, grid_col[:, None] * inverse], axis=-1)
    cosine, sine = jnp.cos(angles), jnp.sin(angles)
    cos_t = jnp.concatenate([cosine] * 4, axis=-1)
    sin_t = jnp.concatenate([-sine, sine, -sine, sine], axis=-1)
    flat = latents.reshape(rows, samples * width)
    flat_ctx = context.reshape(ctx_rows, samples * width)
    if kv_cols % 128:
        projections = (w_query, jnp.concatenate([w_key, w_value], axis=1))
    else:
        projections = (w_query, w_key, w_value)
    dma = pltpu.SemaphoreType.DMA
    q, kv, ctx, gate = pl.pallas_call(
        functools.partial(front_kernel, n_tp, n_sp, samples, q_cols, kv_cols),
        out_shape=(
            jax.ShapeDtypeStruct((samples, tokens, q_cols), BF16),
            jax.ShapeDtypeStruct((samples, tokens + 2 * WINDOW, 2 * kv_cols), BF16),
            jax.ShapeDtypeStruct((n_sp, samples, ctx_rows, 2 * kv_cols), BF16),
            jax.ShapeDtypeStruct((8, width), F32),
        ),
        in_specs=[VMEM] * 4 + [ANY] * (5 + len(projections)),
        out_specs=(VMEM,) * 4,
        scratch_shapes=[
            pltpu.VMEM((n_tp, samples, rows, width), BF16),
            pltpu.VMEM((samples, ctx_rows, width), BF16),
            pltpu.VMEM((3, mod_rows, mw), BF16),
            pltpu.VMEM((width, q_cols + 2 * kv_cols), BF16),
            pltpu.VMEM((8, 3 * mw), F32),
            pltpu.VMEM((n_sp, 8, 3 * mw), F32),
            pltpu.VMEM((n_tp, 8, 3 * mw), F32),
            pltpu.VMEM((8, 3 * width), F32),
            dma((2 * samples + 6,)),
            dma((n_sp,)),
            dma((n_sp,)),
            dma((n_tp,)),
            dma((n_tp,)),
            dma((nx, samples, 2)),
            dma((nx, samples, 2)),
            dma((samples,)),
            dma((samples,)),
            dma((nx, samples)),
            dma((nx, samples)),
            dma((n_sp,)),
            dma((n_sp,)),
            dma((2,)),
            dma((2,)),
        ],
        compiler_params=pltpu.CompilerParams(
            collective_id=0, has_side_effects=True, vmem_limit_bytes=VMEM_LIMIT
        ),
        name="front",
    )(
        lifted,
        norm_gain.reshape(1, width),
        cos_t,
        sin_t,
        flat,
        flat_ctx,
        w_shift,
        w_scale,
        w_gate,
        *projections,
    )
    block = min(tokens, 128)
    att = pl.pallas_call(
        functools.partial(attend_kernel, n_sp, kv_cols, per_group),
        grid=(samples, tokens // block),
        out_shape=jax.ShapeDtypeStruct((samples, tokens, q_cols), BF16),
        in_specs=[
            pl.BlockSpec(memory_space=pltpu.SMEM),
            pl.BlockSpec((1, block, q_cols), lambda s, b: (s, b, 0)),
            pl.BlockSpec((1, tokens + 2 * WINDOW, 2 * kv_cols), lambda s, b: (s, 0, 0)),
            pl.BlockSpec((n_sp, 1, ctx_rows, 2 * kv_cols), lambda s, b: (0, s, 0, 0)),
        ],
        out_specs=pl.BlockSpec((1, block, q_cols), lambda s, b: (s, b, 0)),
        compiler_params=pltpu.CompilerParams(vmem_limit_bytes=VMEM_LIMIT),
        name="attend",
    )(sink_logit, q, kv, ctx)
    out = pl.pallas_call(
        functools.partial(back_kernel, n_tp, samples),
        out_shape=jax.ShapeDtypeStruct((rows, samples * width), BF16),
        in_specs=[VMEM] * 4,
        out_specs=VMEM,
        scratch_shapes=[
            pltpu.VMEM((samples, rows, width), F32),
            pltpu.VMEM((nx, samples, rows, width), BF16),
            pltpu.VMEM((nx, samples, rows, width), BF16),
            pltpu.VMEM((nx, samples, rows, width), BF16),
            pltpu.VMEM((nx, samples, rows, width), BF16),
            dma((nx, samples)),
            dma((nx, samples)),
            dma((nx, samples)),
            dma((nx, samples)),
        ],
        compiler_params=pltpu.CompilerParams(
            collective_id=1, has_side_effects=True, vmem_limit_bytes=VMEM_LIMIT
        ),
        name="back",
    )(att, w_out, gate, flat)
    return out.reshape(rows, samples, width)


def solution(mesh):
    return jax.shard_map(
        on_device,
        mesh=mesh,
        in_specs=(
            P(("sp", "tp"), "grp", None),
            P("sp", "grp", None),
            P("grp", "sp"),
            P("sp"),
            P("sp", "tp"),
            P("sp", "tp"),
            P("sp", "tp"),
            P(),
            P(None, "tp"),
            P(None, "tp"),
            P(None, "tp"),
            P("tp"),
            P("tp", None),
        ),
        out_specs=P(("sp", "tp"), "grp", None),
        check_vma=False,
    )
```

```python
import functools

import jax
import jax.numpy as jnp
import numpy as np
from jax import lax
from jax.experimental import pallas as pl
from jax.experimental.pallas import tpu as pltpu
from jax.sharding import PartitionSpec as P

HEAD_DIM = 64
WINDOW = 128
GRID_W = 64
EPS = 1e-06
THETA = 10000.0
BIG_NEG = -1e30
VMEM_LIMIT = 60 * 1024 * 1024
F32 = jnp.float32
BF16 = jnp.bfloat16
ANY = pl.BlockSpec(memory_space=pl.ANY)
VMEM = pl.BlockSpec(memory_space=pltpu.VMEM)


def enter(peers):
    barrier = pltpu.get_barrier_semaphore()
    for peer in peers:
        pl.semaphore_signal(
            barrier, inc=1, device_id=peer, device_id_type=pl.DeviceIdType.MESH
        )
    pl.semaphore_wait(barrier, len(peers))


def remote(src, dst, send, recv, peer):
    return pltpu.make_async_remote_copy(
        src_ref=src,
        dst_ref=dst,
        send_sem=send,
        recv_sem=recv,
        device_id=peer,
        device_id_type=pl.DeviceIdType.MESH,
    )


def block_kernel(n_tp, n_sp, samples, q_cols, kv_cols, n_proj, *refs):
    cond, cond_ctx, gain, cos_row, sin_row, cos_col, sin_col, sinks = refs[:8]
    lat_hbm, ctx_hbm, ws_hbm, wc_hbm, wg_hbm, wo_hbm = refs[8:14]
    proj_hbm = refs[14 : 14 + n_proj]
    out = refs[14 + n_proj]
    (
        gath,
        ctx_in,
        wm,
        wj,
        wo,
        modp,
        mod_sp,
        mod_all,
        modv,
        cos_t,
        sin_t,
        queries,
        kv,
        ctx_all,
        att,
        arr,
        loc,
        sps,
        spr,
        tps,
        tpr,
        xs,
        xr,
        ps,
        pr,
        rs,
        rr,
        cs,
        cr,
        hs,
        hr,
        avs,
        avr,
    ) = refs[15 + n_proj :]
    nx = n_tp // 2
    rows, width = gath.shape[2], gath.shape[3]
    tokens = rows * n_tp
    mw = wm.shape[2]
    per_group = q_cols // kv_cols
    sp = lax.axis_index("sp")
    tp = lax.axis_index("tp")
    mx, core = tp // 2, lax.rem(tp, 2)
    mate = {"tp": mx * 2 + 1 - core}
    pieces = wo.shape[1]
    wo_rows = wo.shape[2]

    def local(i, src, dst):
        return pltpu.make_async_copy(src, dst, loc.at[i])

    n_loc = 0
    loads, mats, joins, ctxs, outs = [], [], [], [], []
    for s in range(samples):
        loads.append(local(n_loc, lat_hbm.at[:, pl.ds(s * width, width)], gath.at[tp, s]))
        n_loc += 1
    for i, w in enumerate((ws_hbm, wc_hbm, wg_hbm)):
        mats.append(local(n_loc, w, wm.at[i]))
        n_loc += 1
    for s in range(samples):
        ctxs.append(local(n_loc, ctx_hbm.at[:, pl.ds(s * width, width)], ctx_in.at[s]))
        n_loc += 1
    c0 = 0
    for w in proj_hbm:
        joins.append(local(n_loc, w, wj.at[:, pl.ds(c0, w.shape[1])]))
        c0 += w.shape[1]
        n_loc += 1
    for i in range(pieces):
        outs.append(local(n_loc, wo_hbm.at[pl.ds(i * wo_rows, wo_rows)], wo.at[tp, i]))
        n_loc += 1
    for c in loads + mats + ctxs + joins + outs:
        c.start()
    enter(
        [{"tp": lax.rem(tp + d, n_tp)} for d in range(1, n_tp)]
        + [{"sp": lax.rem(sp + d, n_sp)} for d in range(1, n_sp)]
    )

    def spot(owner, i, kind):
        return (wo if kind else gath).at[owner, i]

    def x_send(d, i, kind=0):
        peer = {"tp": lax.rem(mx + d, nx) * 2 + core}
        at = i + kind * samples
        piece = spot(tp, i, kind)
        return remote(piece, piece, xs.at[d, at], xr.at[d, at], peer)

    def mate_send(i, kind=0):
        at = i + kind * samples
        piece = spot(tp, i, kind)
        return remote(piece, piece, ps.at[at], pr.at[at], mate)

    def relay(d, i, kind=0):
        at = i + kind * samples
        piece = spot(lax.rem(mx - d + nx, nx) * 2 + core, i, kind)
        return remote(piece, piece, rs.at[d, at], rr.at[d, at], mate)

    for c in loads:
        c.wait()
    for d in range(1, nx):
        x_send(d, 0).start()
    given = jnp.concatenate(
        [cond[...], cond_ctx[...], jnp.zeros((16 - samples - 1, cond.shape[1]), F32)], axis=0
    )
    lifted = (given / (1.0 + jnp.exp(-given))).astype(BF16)
    for c in mats:
        c.wait()
    for i in range(3):
        part = jnp.dot(lifted, wm[i], preferred_element_type=F32)
        for r in range(samples + 1):
            modp[r, :, i * mw : (i + 1) * mw] = part[r : r + 1]
    sp_sends = [
        remote(modp, mod_sp.at[d], sps.at[d], spr.at[d], {"sp": lax.rem(sp + d, n_sp)})
        for d in range(1, n_sp)
    ]
    for c in sp_sends:
        c.start()
    for s in range(samples):
        mate_send(s).start()
    line = tokens // GRID_W
    axis_row = lax.rem(lax.broadcasted_iota(jnp.int32, (GRID_W, 128), 1), 32) < HEAD_DIM // 4
    for r in range(line):
        cos_t[r * GRID_W : (r + 1) * GRID_W] = jnp.where(
            axis_row, cos_row[pl.ds(sp * line + r, 1), :], cos_col[...]
        )
        sin_t[r * GRID_W : (r + 1) * GRID_W] = jnp.where(
            axis_row, sin_row[pl.ds(sp * line + r, 1), :], sin_col[...]
        )
    for c in sp_sends:
        c.wait()
    total = modp[...]
    for d in range(1, n_sp):
        total = total + mod_sp[d]
    mod_all[tp] = total
    tp_sends = [
        remote(
            mod_all.at[tp],
            mod_all.at[tp],
            tps.at[d],
            tpr.at[d],
            {"tp": lax.rem(tp + d, n_tp)},
        )
        for d in range(1, n_tp)
    ]
    for c in tp_sends:
        c.start()
    for s in range(1, samples):
        for d in range(1, nx):
            x_send(d, s).start()
    for c in outs:
        c.wait()
    for i in range(pieces):
        for d in range(1, nx):
            x_send(d, i, 1).start()
        mate_send(i, 1).start()
    for c in tp_sends:
        c.wait()
    for t in range(n_tp):
        for i in range(3):
            modv[:, :, i * width + t * mw : i * width + (t + 1) * mw] = mod_all[
                t, :, :, i * mw : (i + 1) * mw
            ]
    for r in range(samples + 1):
        modv[r, :, width : 2 * width] = gain[...] * (1.0 + modv[r, :, width : 2 * width])

    def norm(block, row):
        up = block.astype(F32)
        inv = lax.rsqrt(jnp.mean(up * up, axis=-1, keepdims=True) + EPS)
        return (up * inv * modv[row, :, width : 2 * width] + modv[row, :, :width]).astype(BF16)

    for c in joins + ctxs:
        c.wait()

    def ctx_step(s, carry):
        ctx_all[sp, s] = jnp.dot(
            norm(ctx_in[s], samples), wj[:, q_cols:], preferred_element_type=F32
        ).astype(BF16)
        return carry

    lax.fori_loop(0, samples, ctx_step, 0)
    ctx_sends = [
        remote(
            ctx_all.at[sp], ctx_all.at[sp], cs.at[d], cr.at[d], {"sp": lax.rem(sp + d, n_sp)}
        )
        for d in range(1, n_sp)
    ]
    for c in ctx_sends:
        c.start()
    scale = HEAD_DIM**-0.5
    lane = lax.broadcasted_iota(jnp.int32, (rows, 128), 1)
    low = lax.rem(lane, HEAD_DIM) < HEAD_DIM // 2

    def project(owner, s):
        at = pl.multiple_of(owner * rows, rows)
        res = jnp.dot(norm(gath[owner, s], s), wj[...], preferred_element_type=F32)
        cosine = cos_t[pl.ds(at, rows), :]
        sine = sin_t[pl.ds(at, rows), :]
        for c0 in range(0, q_cols + 2 * kv_cols, 128):
            part = res[:, c0 : c0 + 128]
            turned = part
            if c0 < q_cols + kv_cols:
                swapped = jnp.where(low, pltpu.roll(part, 96, 1), pltpu.roll(part, 32, 1))
                turned = part * cosine + swapped * sine
            if c0 < q_cols:
                queries[s, pl.ds(at, rows), c0 : c0 + 128] = (turned * scale).astype(BF16)
            else:
                if c0 + 128 > q_cols + kv_cols and c0 < q_cols + kv_cols:
                    turned = jnp.where(lane < q_cols + kv_cols - c0, turned, part)
                kv[s, pl.ds(WINDOW + at, rows), c0 - q_cols : c0 - q_cols + 128] = turned.astype(
                    BF16
                )

    up_edge = sp == n_sp - 1
    down_edge = sp == 0

    def halo_up(s):
        return remote(
            kv.at[s, pl.ds(tokens, WINDOW)],
            kv.at[s, pl.ds(0, WINDOW)],
            hs.at[0, s],
            hr.at[0, s],
            {"sp": lax.rem(sp + 1, n_sp)},
        )

    def halo_down(s):
        return remote(
            kv.at[s, pl.ds(WINDOW, WINDOW)],
            kv.at[s, pl.ds(tokens + WINDOW, WINDOW)],
            hs.at[1, s],
            hr.at[1, s],
            {"sp": lax.rem(sp + n_sp - 1, n_sp)},
        )

    zero = jnp.zeros((WINDOW, 2 * kv_cols), BF16)

    def sample_step(s, carry):
        def own_and_mate(k, inner):
            @pl.when(k == 1)
            def _():
                mate_send(s).wait_recv()

            project(lax.rem(tp + 0, n_tp) * (1 - k) + (mx * 2 + 1 - core) * k, s)
            return inner

        lax.fori_loop(0, 2, own_and_mate, 0)
        for d in range(1, nx):
            x_send(d, s).wait_recv()
            relay(d, s).start()

        def crossed(k, inner):
            d = 1 + k // 2
            far = lax.rem(k, 2)

            @pl.when(far == 1)
            def _():
                relay(d, s).wait_recv()

            side = core * (1 - far) + (1 - core) * far
            project(lax.rem(mx - d + nx, nx) * 2 + side, s)
            return inner

        lax.fori_loop(0, 2 * (nx - 1), crossed, 0)

        @pl.when(jnp.logical_not(up_edge))
        def _():
            halo_up(s).start()

        @pl.when(jnp.logical_not(down_edge))
        def _():
            halo_down(s).start()

        @pl.when(up_edge)
        def _():
            kv[s, tokens + WINDOW :, :] = zero

        @pl.when(down_edge)
        def _():
            kv[s, :WINDOW, :] = zero

        return carry

    lax.fori_loop(0, samples, sample_step, 0)
    for c in ctx_sends:
        c.wait()
    q_rows = min(tokens, 128)
    span = q_rows + 2 * WINDOW
    stacked = per_group * q_rows
    contract = (((1,), (1,)), ((), ()))

    def attend(s, block):
        at = pl.multiple_of(block * q_rows, q_rows)
        window = kv[s, pl.ds(at, span), :]
        ctx = ctx_all[:, s].reshape(-1, 2 * kv_cols)
        q_all = queries[s, pl.ds(at, q_rows), :]
        row = lax.rem(lax.broadcasted_iota(jnp.int32, (stacked, span), 0), q_rows)
        col = lax.broadcasted_iota(jnp.int32, (stacked, span), 1)
        k_pos = sp * tokens + at - WINDOW + col
        keep = (col >= row) & (col <= row + 2 * WINDOW) & (k_pos >= 0) & (k_pos < n_sp * tokens)
        first = lax.broadcasted_iota(jnp.int32, (stacked, 1), 0)
        for g in range(kv_cols // HEAD_DIM):
            heads = range(g * per_group, (g + 1) * per_group)
            q = jnp.concatenate(
                [q_all[:, h * HEAD_DIM : (h + 1) * HEAD_DIM] for h in heads], axis=0
            )
            sink = jnp.full((stacked, 1), sinks[g * per_group], F32)
            for j in range(1, per_group):
                sink = jnp.where(first >= j * q_rows, sinks[g * per_group + j], sink)
            ks = slice(g * HEAD_DIM, (g + 1) * HEAD_DIM)
            vs = slice(kv_cols + g * HEAD_DIM, kv_cols + (g + 1) * HEAD_DIM)
            near = lax.dot_general(q, window[:, ks], contract, preferred_element_type=F32)
            near = jnp.where(keep, near, BIG_NEG)
            far = lax.dot_general(q, ctx[:, ks], contract, preferred_element_type=F32)
            top = jnp.maximum(
                jnp.maximum(
                    jnp.max(near, axis=-1, keepdims=True), jnp.max(far, axis=-1, keepdims=True)
                ),
                sink,
            )
            near = jnp.exp(near - top)
            far = jnp.exp(far - top)
            below = (
                jnp.sum(near, axis=-1, keepdims=True)
                + jnp.sum(far, axis=-1, keepdims=True)
                + jnp.exp(sink - top)
            )
            mixed = jnp.dot(near.astype(BF16), window[:, vs], preferred_element_type=F32)
            mixed = mixed + jnp.dot(far.astype(BF16), ctx[:, vs], preferred_element_type=F32)
            mixed = (mixed / below).astype(BF16)
            for j, h in enumerate(heads):
                att[s, pl.ds(at, q_rows), h * HEAD_DIM : (h + 1) * HEAD_DIM] = mixed[
                    j * q_rows : (j + 1) * q_rows
                ]

    def swap(d, s):
        to = lax.rem(tp + d, n_tp)
        at = pl.multiple_of(to * rows, rows)
        return remote(
            att.at[s, pl.ds(at, rows)], arr.at[s, tp], avs.at[d, s], avr.at[d, s], {"tp": to}
        )

    def attend_step(s, carry):
        @pl.when(jnp.logical_not(down_edge))
        def _():
            halo_up(s).wait_recv()

        @pl.when(jnp.logical_not(up_edge))
        def _():
            halo_down(s).wait_recv()

        def one(block, inner):
            attend(s, block)
            return inner

        lax.fori_loop(0, tokens // q_rows, one, 0)
        for d in range(1, n_tp):
            swap(d, s).start()
        arr[s, tp] = att[s, pl.ds(pl.multiple_of(tp * rows, rows), rows), :]
        return carry

    lax.fori_loop(0, samples, attend_step, 0)
    for i in range(pieces):
        for d in range(1, nx):
            x_send(d, i, 1).wait_recv()
            relay(d, i, 1).start()
    for i in range(pieces):
        mate_send(i, 1).wait_recv()
        for d in range(1, nx):
            relay(d, i, 1).wait_recv()

    for s in range(samples):
        for d in range(1, n_tp):
            swap(d, s).wait_recv()
        cols = slice(s * width, (s + 1) * width)
        lhs = jnp.concatenate([arr[s, t] for t in range(n_tp)], axis=1)
        mixed = jnp.dot(lhs, wo[...].reshape(-1, width), preferred_element_type=F32)
        gate = modv[s, :, 2 * width :]
        out[:, cols] = (gath[tp, s].astype(F32) + gate * mixed).astype(BF16)

    for s in range(samples):
        for d in range(1, n_tp):
            swap(d, s).wait_send()
        mate_send(s).wait_send()
        for d in range(1, nx):
            x_send(d, s).wait_send()
            relay(d, s).wait_send()

        @pl.when(jnp.logical_not(up_edge))
        def _():
            halo_up(s).wait_send()

        @pl.when(jnp.logical_not(down_edge))
        def _():
            halo_down(s).wait_send()

    for i in range(pieces):
        mate_send(i, 1).wait_send()
        for d in range(1, nx):
            x_send(d, i, 1).wait_send()
            relay(d, i, 1).wait_send()


def rope_tables(lines):
    quarter = HEAD_DIM // 4
    inverse = THETA ** (-np.arange(quarter) / quarter)
    tables = []
    for count in (lines, GRID_W):
        angles = np.tile(np.arange(count)[:, None] * inverse, (1, 8))
        sign = np.where(np.arange(128) % HEAD_DIM < HEAD_DIM // 2, -1.0, 1.0)
        tables.append(jnp.asarray(np.cos(angles), F32))
        tables.append(jnp.asarray(np.sin(angles) * sign, F32))
    return tables


def on_device(
    latents,
    context,
    condition,
    cond_context,
    w_shift,
    w_scale,
    w_gate,
    norm_gain,
    w_query,
    w_key,
    w_value,
    sink_logit,
    w_out,
):
    rows, samples, width = latents.shape
    n_tp = lax.axis_size("tp")
    n_sp = lax.axis_size("sp")
    nx = n_tp // 2
    tokens = rows * n_tp
    q_cols = w_query.shape[1]
    kv_cols = w_key.shape[1]
    ctx_rows = context.shape[0]
    mod_rows, mw = w_shift.shape
    pieces = 2
    flat = latents.reshape(rows, samples * width)
    flat_ctx = context.reshape(ctx_rows, samples * width)
    if kv_cols % 128:
        projections = (w_query, jnp.concatenate([w_key, w_value], axis=1))
    else:
        projections = (w_query, w_key, w_value)
    tables = rope_tables(n_sp * tokens // GRID_W)
    dma = pltpu.SemaphoreType.DMA
    n_move = samples + pieces
    out = pl.pallas_call(
        functools.partial(
            block_kernel, n_tp, n_sp, samples, q_cols, kv_cols, len(projections)
        ),
        out_shape=jax.ShapeDtypeStruct((rows, samples * width), BF16),
        in_specs=[VMEM] * 7
        + [pl.BlockSpec(memory_space=pltpu.SMEM)]
        + [ANY] * (6 + len(projections)),
        out_specs=VMEM,
        scratch_shapes=[
            pltpu.VMEM((n_tp, samples, rows, width), BF16),
            pltpu.VMEM((samples, ctx_rows, width), BF16),
            pltpu.VMEM((3, mod_rows, mw), BF16),
            pltpu.VMEM((width, q_cols + 2 * kv_cols), BF16),
            pltpu.VMEM((n_tp, pieces, q_cols // pieces, width), BF16),
            pltpu.VMEM((samples + 1, 1, 3 * mw), F32),
            pltpu.VMEM((n_sp, samples + 1, 1, 3 * mw), F32),
            pltpu.VMEM((n_tp, samples + 1, 1, 3 * mw), F32),
            pltpu.VMEM((samples + 1, 1, 3 * width), F32),
            pltpu.VMEM((tokens, 128), F32),
            pltpu.VMEM((tokens, 128), F32),
            pltpu.VMEM((samples, tokens, q_cols), BF16),
            pltpu.VMEM((samples, tokens + 2 * WINDOW, 2 * kv_cols), BF16),
            pltpu.VMEM((n_sp, samples, ctx_rows, 2 * kv_cols), BF16),
            pltpu.VMEM((samples, tokens, q_cols), BF16),
            pltpu.VMEM((samples, n_tp, rows, q_cols), BF16),
            dma((2 * samples + 6 + pieces,)),
            dma((n_sp,)),
            dma((n_sp,)),
            dma((n_tp,)),
            dma((n_tp,)),
            dma((nx, n_move)),
            dma((nx, n_move)),
            dma((n_move,)),
            dma((n_move,)),
            dma((nx, n_move)),
            dma((nx, n_move)),
            dma((n_sp,)),
            dma((n_sp,)),
            dma((2, samples)),
            dma((2, samples)),
            dma((n_tp, samples)),
            dma((n_tp, samples)),
        ],
        compiler_params=pltpu.CompilerParams(
            collective_id=0, has_side_effects=True, vmem_limit_bytes=VMEM_LIMIT
        ),
        name="block",
    )(
        condition,
        cond_context.reshape(1, -1),
        norm_gain.reshape(1, width),
        *tables,
        sink_logit,
        flat,
        flat_ctx,
        w_shift,
        w_scale,
        w_gate,
        w_out,
        *projections,
    )
    return out.reshape(rows, samples, width)


def solution(mesh):
    return jax.shard_map(
        on_device,
        mesh=mesh,
        in_specs=(
            P(("sp", "tp"), "grp", None),
            P("sp", "grp", None),
            P("grp", "sp"),
            P("sp"),
            P("sp", "tp"),
            P("sp", "tp"),
            P("sp", "tp"),
            P(),
            P(None, "tp"),
            P(None, "tp"),
            P(None, "tp"),
            P("tp"),
            P("tp", None),
        ),
        out_specs=P(("sp", "tp"), "grp", None),
        check_vma=False,
    )
```

```python
import functools

import jax
import jax.numpy as jnp
import numpy as np
from jax import lax
from jax.experimental import pallas as pl
from jax.experimental.pallas import tpu as pltpu
from jax.sharding import PartitionSpec as P

HEAD_DIM = 64
WINDOW = 128
GRID_W = 64
EPS = 1e-06
THETA = 10000.0
BIG_NEG = -1e30
VMEM_LIMIT = 60 * 1024 * 1024
F32 = jnp.float32
BF16 = jnp.bfloat16
ANY = pl.BlockSpec(memory_space=pl.ANY)
VMEM = pl.BlockSpec(memory_space=pltpu.VMEM)


def enter(peers):
    barrier = pltpu.get_barrier_semaphore()
    for peer in peers:
        pl.semaphore_signal(
            barrier, inc=1, device_id=peer, device_id_type=pl.DeviceIdType.MESH
        )
    pl.semaphore_wait(barrier, len(peers))


def remote(src, dst, send, recv, peer):
    return pltpu.make_async_remote_copy(
        src_ref=src,
        dst_ref=dst,
        send_sem=send,
        recv_sem=recv,
        device_id=peer,
        device_id_type=pl.DeviceIdType.MESH,
    )


def block_kernel(n_tp, n_sp, samples, q_cols, kv_cols, n_proj, *refs):
    cond, cond_ctx, gain, cos_row, sin_row, cos_col, sin_col, sinks = refs[:8]
    lat_hbm, ctx_hbm, ws_hbm, wc_hbm, wg_hbm, wo_hbm = refs[8:14]
    proj_hbm = refs[14 : 14 + n_proj]
    out = refs[14 + n_proj]
    (
        gath,
        ctx_in,
        wm,
        wj,
        wo,
        modp,
        mod_sp,
        mod_all,
        modv,
        cos_t,
        sin_t,
        queries,
        kv,
        ctx_all,
        att,
        arr,
        loc,
        sps,
        spr,
        tps,
        tpr,
        xs,
        xr,
        ps,
        pr,
        rs,
        rr,
        cs,
        cr,
        hs,
        hr,
        avs,
        avr,
        ys,
        yr,
    ) = refs[15 + n_proj :]
    nx = n_tp // 2
    rows, width = gath.shape[2], gath.shape[3]
    tokens = rows * n_tp
    mw = wm.shape[2]
    per_group = q_cols // kv_cols
    sp = lax.axis_index("sp")
    tp = lax.axis_index("tp")
    grp = lax.axis_index("grp")
    mx, core = tp // 2, lax.rem(tp, 2)
    mate = {"tp": mx * 2 + 1 - core}
    n_grp = wo.shape[1] // samples
    pieces = wo.shape[1]
    wo_rows = wo.shape[2]

    def local(i, src, dst):
        return pltpu.make_async_copy(src, dst, loc.at[i])

    n_loc = 0
    loads, mats, joins, ctxs, outs = [], [], [], [], []
    for s in range(samples):
        loads.append(local(n_loc, lat_hbm.at[:, pl.ds(s * width, width)], gath.at[tp, s]))
        n_loc += 1
    for i, w in enumerate((ws_hbm, wc_hbm, wg_hbm)):
        mats.append(local(n_loc, w, wm.at[i]))
        n_loc += 1
    for s in range(samples):
        ctxs.append(local(n_loc, ctx_hbm.at[:, pl.ds(s * width, width)], ctx_in.at[s]))
        n_loc += 1
    c0 = 0
    for w in proj_hbm:
        joins.append(local(n_loc, w, wj.at[:, pl.ds(c0, w.shape[1])]))
        c0 += w.shape[1]
        n_loc += 1
    for i in range(pieces):
        outs.append(local(n_loc, wo_hbm.at[pl.ds(i * wo_rows, wo_rows)], wo.at[tp, i]))
        n_loc += 1
    for c in loads + mats + ctxs + joins + outs:
        c.start()
    enter(
        [{"tp": lax.rem(tp + d, n_tp)} for d in range(1, n_tp)]
        + [{"sp": lax.rem(sp + d, n_sp)} for d in range(1, n_sp)]
        + [{"grp": lax.rem(grp + d, n_grp)} for d in range(1, n_grp)]
    )

    def spot(owner, i, kind):
        return (wo if kind else gath).at[owner, i]

    def x_send(d, i, kind=0):
        peer = {"tp": lax.rem(mx + d, nx) * 2 + core}
        at = i + kind * samples
        piece = spot(tp, i, kind)
        return remote(piece, piece, xs.at[d, at], xr.at[d, at], peer)

    def mate_send(i, kind=0):
        at = i + kind * samples
        piece = spot(tp, i, kind)
        return remote(piece, piece, ps.at[at], pr.at[at], mate)

    def relay(d, i, kind=0):
        at = i + kind * samples
        piece = spot(lax.rem(mx - d + nx, nx) * 2 + core, i, kind)
        return remote(piece, piece, rs.at[d, at], rr.at[d, at], mate)

    def share(e, k):
        return lax.rem(grp - e + n_grp, n_grp) * samples + k

    def y_send(d, e, k):
        piece = spot(lax.rem(mx - d + nx, nx) * 2 + core, share(0, k), 1)
        peer = {"grp": lax.rem(grp + e, n_grp)}
        return remote(piece, piece, ys.at[d, e, k], yr.at[d, e, k], peer)

    for c in loads:
        c.wait()
    for d in range(1, nx):
        x_send(d, 0).start()
    given = jnp.concatenate(
        [cond[...], cond_ctx[...], jnp.zeros((16 - samples - 1, cond.shape[1]), F32)], axis=0
    )
    lifted = (given / (1.0 + jnp.exp(-given))).astype(BF16)
    for c in mats:
        c.wait()
    for i in range(3):
        part = jnp.dot(lifted, wm[i], preferred_element_type=F32)
        for r in range(samples + 1):
            modp[r, :, i * mw : (i + 1) * mw] = part[r : r + 1]
    sp_sends = [
        remote(modp, mod_sp.at[d], sps.at[d], spr.at[d], {"sp": lax.rem(sp + d, n_sp)})
        for d in range(1, n_sp)
    ]
    for c in sp_sends:
        c.start()
    for s in range(samples):
        mate_send(s).start()
    line = tokens // GRID_W
    axis_row = lax.rem(lax.broadcasted_iota(jnp.int32, (GRID_W, 128), 1), 32) < HEAD_DIM // 4
    for r in range(line):
        cos_t[r * GRID_W : (r + 1) * GRID_W] = jnp.where(
            axis_row, cos_row[pl.ds(sp * line + r, 1), :], cos_col[...]
        )
        sin_t[r * GRID_W : (r + 1) * GRID_W] = jnp.where(
            axis_row, sin_row[pl.ds(sp * line + r, 1), :], sin_col[...]
        )
    for c in sp_sends:
        c.wait()
    total = modp[...]
    for d in range(1, n_sp):
        total = total + mod_sp[d]
    mod_all[tp] = total
    tp_sends = [
        remote(
            mod_all.at[tp],
            mod_all.at[tp],
            tps.at[d],
            tpr.at[d],
            {"tp": lax.rem(tp + d, n_tp)},
        )
        for d in range(1, n_tp)
    ]
    for c in tp_sends:
        c.start()
    for s in range(1, samples):
        for d in range(1, nx):
            x_send(d, s).start()
    for c in outs:
        c.wait()
    for k in range(samples):
        for d in range(1, nx):
            x_send(d, share(0, k), 1).start()
    for i in range(pieces):
        mate_send(i, 1).start()
    for c in tp_sends:
        c.wait()
    for t in range(n_tp):
        for i in range(3):
            modv[:, :, i * width + t * mw : i * width + (t + 1) * mw] = mod_all[
                t, :, :, i * mw : (i + 1) * mw
            ]
    for r in range(samples + 1):
        modv[r, :, width : 2 * width] = gain[...] * (1.0 + modv[r, :, width : 2 * width])

    def norm(block, row):
        up = block.astype(F32)
        inv = lax.rsqrt(jnp.mean(up * up, axis=-1, keepdims=True) + EPS)
        return (up * inv * modv[row, :, width : 2 * width] + modv[row, :, :width]).astype(BF16)

    for c in joins + ctxs:
        c.wait()

    def ctx_step(s, carry):
        ctx_all[sp, s] = jnp.dot(
            norm(ctx_in[s], samples), wj[:, q_cols:], preferred_element_type=F32
        ).astype(BF16)
        return carry

    lax.fori_loop(0, samples, ctx_step, 0)
    ctx_sends = [
        remote(
            ctx_all.at[sp], ctx_all.at[sp], cs.at[d], cr.at[d], {"sp": lax.rem(sp + d, n_sp)}
        )
        for d in range(1, n_sp)
    ]
    for c in ctx_sends:
        c.start()
    scale = HEAD_DIM**-0.5
    lane = lax.broadcasted_iota(jnp.int32, (rows, 128), 1)
    low = lax.rem(lane, HEAD_DIM) < HEAD_DIM // 2

    def project(owner, s):
        at = pl.multiple_of(owner * rows, rows)
        res = jnp.dot(norm(gath[owner, s], s), wj[...], preferred_element_type=F32)
        cosine = cos_t[pl.ds(at, rows), :]
        sine = sin_t[pl.ds(at, rows), :]
        for c0 in range(0, q_cols + 2 * kv_cols, 128):
            part = res[:, c0 : c0 + 128]
            turned = part
            if c0 < q_cols + kv_cols:
                swapped = jnp.where(low, pltpu.roll(part, 96, 1), pltpu.roll(part, 32, 1))
                turned = part * cosine + swapped * sine
            if c0 < q_cols:
                queries[s, pl.ds(at, rows), c0 : c0 + 128] = (turned * scale).astype(BF16)
            else:
                if c0 + 128 > q_cols + kv_cols and c0 < q_cols + kv_cols:
                    turned = jnp.where(lane < q_cols + kv_cols - c0, turned, part)
                kv[s, pl.ds(WINDOW + at, rows), c0 - q_cols : c0 - q_cols + 128] = turned.astype(
                    BF16
                )

    up_edge = sp == n_sp - 1
    down_edge = sp == 0

    def halo_up(s):
        return remote(
            kv.at[s, pl.ds(tokens, WINDOW)],
            kv.at[s, pl.ds(0, WINDOW)],
            hs.at[0, s],
            hr.at[0, s],
            {"sp": lax.rem(sp + 1, n_sp)},
        )

    def halo_down(s):
        return remote(
            kv.at[s, pl.ds(WINDOW, WINDOW)],
            kv.at[s, pl.ds(tokens + WINDOW, WINDOW)],
            hs.at[1, s],
            hr.at[1, s],
            {"sp": lax.rem(sp + n_sp - 1, n_sp)},
        )

    zero = jnp.zeros((WINDOW, 2 * kv_cols), BF16)

    def sample_step(s, carry):
        def own_and_mate(k, inner):
            @pl.when(k == 1)
            def _():
                mate_send(s).wait_recv()

            project(lax.rem(tp + 0, n_tp) * (1 - k) + (mx * 2 + 1 - core) * k, s)
            return inner

        lax.fori_loop(0, 2, own_and_mate, 0)
        for d in range(1, nx):
            x_send(d, s).wait_recv()
            relay(d, s).start()

        def crossed(k, inner):
            d = 1 + k // 2
            far = lax.rem(k, 2)

            @pl.when(far == 1)
            def _():
                relay(d, s).wait_recv()

            side = core * (1 - far) + (1 - core) * far
            project(lax.rem(mx - d + nx, nx) * 2 + side, s)
            return inner

        lax.fori_loop(0, 2 * (nx - 1), crossed, 0)

        @pl.when(jnp.logical_not(up_edge))
        def _():
            halo_up(s).start()

        @pl.when(jnp.logical_not(down_edge))
        def _():
            halo_down(s).start()

        @pl.when(up_edge)
        def _():
            kv[s, tokens + WINDOW :, :] = zero

        @pl.when(down_edge)
        def _():
            kv[s, :WINDOW, :] = zero

        return carry

    lax.fori_loop(0, samples, sample_step, 0)
    for c in ctx_sends:
        c.wait()
    q_rows = min(tokens, 128)
    span = q_rows + 2 * WINDOW
    stacked = per_group * q_rows
    contract = (((1,), (1,)), ((), ()))

    def attend(s, block):
        at = pl.multiple_of(block * q_rows, q_rows)
        window = kv[s, pl.ds(at, span), :]
        ctx = ctx_all[:, s].reshape(-1, 2 * kv_cols)
        q_all = queries[s, pl.ds(at, q_rows), :]
        row = lax.rem(lax.broadcasted_iota(jnp.int32, (stacked, span), 0), q_rows)
        col = lax.broadcasted_iota(jnp.int32, (stacked, span), 1)
        k_pos = sp * tokens + at - WINDOW + col
        keep = (col >= row) & (col <= row + 2 * WINDOW) & (k_pos >= 0) & (k_pos < n_sp * tokens)
        first = lax.broadcasted_iota(jnp.int32, (stacked, 1), 0)
        for g in range(kv_cols // HEAD_DIM):
            heads = range(g * per_group, (g + 1) * per_group)
            q = jnp.concatenate(
                [q_all[:, h * HEAD_DIM : (h + 1) * HEAD_DIM] for h in heads], axis=0
            )
            sink = jnp.full((stacked, 1), sinks[g * per_group], F32)
            for j in range(1, per_group):
                sink = jnp.where(first >= j * q_rows, sinks[g * per_group + j], sink)
            ks = slice(g * HEAD_DIM, (g + 1) * HEAD_DIM)
            vs = slice(kv_cols + g * HEAD_DIM, kv_cols + (g + 1) * HEAD_DIM)
            near = lax.dot_general(q, window[:, ks], contract, preferred_element_type=F32)
            near = jnp.where(keep, near, BIG_NEG)
            far = lax.dot_general(q, ctx[:, ks], contract, preferred_element_type=F32)
            top = jnp.maximum(
                jnp.maximum(
                    jnp.max(near, axis=-1, keepdims=True), jnp.max(far, axis=-1, keepdims=True)
                ),
                sink,
            )
            near = jnp.exp(near - top)
            far = jnp.exp(far - top)
            below = (
                jnp.sum(near, axis=-1, keepdims=True)
                + jnp.sum(far, axis=-1, keepdims=True)
                + jnp.exp(sink - top)
            )
            mixed = jnp.dot(near.astype(BF16), window[:, vs], preferred_element_type=F32)
            mixed = mixed + jnp.dot(far.astype(BF16), ctx[:, vs], preferred_element_type=F32)
            mixed = (mixed / below).astype(BF16)
            for j, h in enumerate(heads):
                att[s, pl.ds(at, q_rows), h * HEAD_DIM : (h + 1) * HEAD_DIM] = mixed[
                    j * q_rows : (j + 1) * q_rows
                ]

    def swap(d, s):
        to = lax.rem(tp + d, n_tp)
        at = pl.multiple_of(to * rows, rows)
        return remote(
            att.at[s, pl.ds(at, rows)], arr.at[s, tp], avs.at[d, s], avr.at[d, s], {"tp": to}
        )

    def attend_step(s, carry):
        @pl.when(jnp.logical_not(down_edge))
        def _():
            halo_up(s).wait_recv()

        @pl.when(jnp.logical_not(up_edge))
        def _():
            halo_down(s).wait_recv()

        def one(block, inner):
            @pl.when(block == tokens // q_rows // 2)
            def _():
                for d in range(1, nx):
                    x_send(d, share(0, s), 1).wait_recv()
                    for e in range(1, n_grp):
                        y_send(d, e, s).start()
                    relay(d, share(0, s), 1).start()

            attend(s, block)
            return inner

        lax.fori_loop(0, tokens // q_rows, one, 0)
        for d in range(1, n_tp):
            swap(d, s).start()
        arr[s, tp] = att[s, pl.ds(pl.multiple_of(tp * rows, rows), rows), :]
        return carry

    lax.fori_loop(0, samples, attend_step, 0)
    for k in range(samples):
        for d in range(1, nx):
            for e in range(1, n_grp):
                y_send(d, e, k).wait_recv()
                relay(d, share(e, k), 1).start()
    for i in range(pieces):
        mate_send(i, 1).wait_recv()
        for d in range(1, nx):
            relay(d, i, 1).wait_recv()

    for s in range(samples):
        for d in range(1, n_tp):
            swap(d, s).wait_recv()
        cols = slice(s * width, (s + 1) * width)
        lhs = jnp.concatenate([arr[s, t] for t in range(n_tp)], axis=1)
        mixed = jnp.dot(lhs, wo[...].reshape(-1, width), preferred_element_type=F32)
        gate = modv[s, :, 2 * width :]
        out[:, cols] = (gath[tp, s].astype(F32) + gate * mixed).astype(BF16)

    for s in range(samples):
        for d in range(1, n_tp):
            swap(d, s).wait_send()
        mate_send(s).wait_send()
        for d in range(1, nx):
            x_send(d, s).wait_send()
            relay(d, s).wait_send()

        @pl.when(jnp.logical_not(up_edge))
        def _():
            halo_up(s).wait_send()

        @pl.when(jnp.logical_not(down_edge))
        def _():
            halo_down(s).wait_send()

    for k in range(samples):
        for d in range(1, nx):
            x_send(d, share(0, k), 1).wait_send()
            for e in range(1, n_grp):
                y_send(d, e, k).wait_send()
    for i in range(pieces):
        mate_send(i, 1).wait_send()
        for d in range(1, nx):
            relay(d, i, 1).wait_send()


def rope_tables(lines):
    quarter = HEAD_DIM // 4
    inverse = THETA ** (-np.arange(quarter) / quarter)
    tables = []
    for count in (lines, GRID_W):
        angles = np.tile(np.arange(count)[:, None] * inverse, (1, 8))
        sign = np.where(np.arange(128) % HEAD_DIM < HEAD_DIM // 2, -1.0, 1.0)
        tables.append(jnp.asarray(np.cos(angles), F32))
        tables.append(jnp.asarray(np.sin(angles) * sign, F32))
    return tables


def on_device(
    latents,
    context,
    condition,
    cond_context,
    w_shift,
    w_scale,
    w_gate,
    norm_gain,
    w_query,
    w_key,
    w_value,
    sink_logit,
    w_out,
):
    rows, samples, width = latents.shape
    n_tp = lax.axis_size("tp")
    n_sp = lax.axis_size("sp")
    nx = n_tp // 2
    tokens = rows * n_tp
    q_cols = w_query.shape[1]
    kv_cols = w_key.shape[1]
    ctx_rows = context.shape[0]
    mod_rows, mw = w_shift.shape
    pieces = lax.axis_size("grp") * samples
    flat = latents.reshape(rows, samples * width)
    flat_ctx = context.reshape(ctx_rows, samples * width)
    if kv_cols % 128:
        projections = (w_query, jnp.concatenate([w_key, w_value], axis=1))
    else:
        projections = (w_query, w_key, w_value)
    tables = rope_tables(n_sp * tokens // GRID_W)
    dma = pltpu.SemaphoreType.DMA
    n_move = samples + pieces
    out = pl.pallas_call(
        functools.partial(
            block_kernel, n_tp, n_sp, samples, q_cols, kv_cols, len(projections)
        ),
        out_shape=jax.ShapeDtypeStruct((rows, samples * width), BF16),
        in_specs=[VMEM] * 7
        + [pl.BlockSpec(memory_space=pltpu.SMEM)]
        + [ANY] * (6 + len(projections)),
        out_specs=VMEM,
        scratch_shapes=[
            pltpu.VMEM((n_tp, samples, rows, width), BF16),
            pltpu.VMEM((samples, ctx_rows, width), BF16),
            pltpu.VMEM((3, mod_rows, mw), BF16),
            pltpu.VMEM((width, q_cols + 2 * kv_cols), BF16),
            pltpu.VMEM((n_tp, pieces, q_cols // pieces, width), BF16),
            pltpu.VMEM((samples + 1, 1, 3 * mw), F32),
            pltpu.VMEM((n_sp, samples + 1, 1, 3 * mw), F32),
            pltpu.VMEM((n_tp, samples + 1, 1, 3 * mw), F32),
            pltpu.VMEM((samples + 1, 1, 3 * width), F32),
            pltpu.VMEM((tokens, 128), F32),
            pltpu.VMEM((tokens, 128), F32),
            pltpu.VMEM((samples, tokens, q_cols), BF16),
            pltpu.VMEM((samples, tokens + 2 * WINDOW, 2 * kv_cols), BF16),
            pltpu.VMEM((n_sp, samples, ctx_rows, 2 * kv_cols), BF16),
            pltpu.VMEM((samples, tokens, q_cols), BF16),
            pltpu.VMEM((samples, n_tp, rows, q_cols), BF16),
            dma((2 * samples + 6 + pieces,)),
            dma((n_sp,)),
            dma((n_sp,)),
            dma((n_tp,)),
            dma((n_tp,)),
            dma((nx, n_move)),
            dma((nx, n_move)),
            dma((n_move,)),
            dma((n_move,)),
            dma((nx, n_move)),
            dma((nx, n_move)),
            dma((n_sp,)),
            dma((n_sp,)),
            dma((2, samples)),
            dma((2, samples)),
            dma((n_tp, samples)),
            dma((n_tp, samples)),
            dma((nx, pieces // samples, samples)),
            dma((nx, pieces // samples, samples)),
        ],
        compiler_params=pltpu.CompilerParams(
            collective_id=0, has_side_effects=True, vmem_limit_bytes=VMEM_LIMIT
        ),
        name="block",
    )(
        condition,
        cond_context.reshape(1, -1),
        norm_gain.reshape(1, width),
        *tables,
        sink_logit,
        flat,
        flat_ctx,
        w_shift,
        w_scale,
        w_gate,
        w_out,
        *projections,
    )
    return out.reshape(rows, samples, width)


def solution(mesh):
    return jax.shard_map(
        on_device,
        mesh=mesh,
        in_specs=(
            P(("sp", "tp"), "grp", None),
            P("sp", "grp", None),
            P("grp", "sp"),
            P("sp"),
            P("sp", "tp"),
            P("sp", "tp"),
            P("sp", "tp"),
            P(),
            P(None, "tp"),
            P(None, "tp"),
            P(None, "tp"),
            P("tp"),
            P("tp", None),
        ),
        out_specs=P(("sp", "tp"), "grp", None),
        check_vma=False,
    )
```
